32 devices in a mesh: grp: 2 (over y), sp: 8 (over z, core), tp: 2 (over x).
Axes of the slice: x: 2, y: 2, z: 4, core: 2. Of those that a mesh axis runs over, the one named last changes fastest.
Arguments:
- resid: bfloat16 [3072, 2048], P(('grp', 'sp', 'tp')), parts along dimension 0, may hold values from -6 to 6
- queries: bfloat16 [3072, 1024], P(('grp', 'sp'), 'tp'), parts along dimension 0, may hold values from -64 to 64
- keys: bfloat16 [3072, 256], P(('grp', 'sp'), 'tp'), parts along dimension 0, may hold values from -64 to 64
- values: bfloat16 [3072, 256], P(('grp', 'sp'), 'tp'), parts along dimension 0, may hold values from -6 to 6
- doc_ids: int32 [3072], P(('grp', 'sp')), parts along dimension 0, may hold values from 0 to 3, never falling along the last dimension, each value on 1 to 768 neighbouring positions
- sink_logits: float32 [16], P('tp'), may hold values from 2 to 6
- out_proj: bfloat16 [1024, 2048], P('tp'), may hold values from -1.5 to 1.5
- norm1_gain: float32 [2048], replicated, may hold values from 0.1 to 1.9
- norm1_bias: float32 [2048], replicated, may hold values from -1.8 to 1.8
- route_ids: int32 [3072, 2], P(('grp', 'sp', 'tp')), parts along dimension 0, may hold values from 0 to 7, all different within a row; in each aligned block of 96 rows (0 to 95, 96 to 191, ...) at most 30 rows name the same one
- route_weights: float32 [3072, 2], P(('grp', 'sp', 'tp')), parts along dimension 0, may hold values from 0.25 to 1
- expert_gate: bfloat16 [8, 2048, 3072], P('sp', None, 'tp'), may hold values from -0.125 to 0.125
- expert_up: bfloat16 [8, 2048, 3072], P('sp', None, 'tp'), may hold values from -0.125 to 0.125
- expert_down: bfloat16 [8, 3072, 2048], P('sp', 'tp'), may hold values from -0.109375 to 0.109375
- norm2_gain: float32 [2048], replicated, may hold values from 0.1 to 1.9
- norm2_bias: float32 [2048], replicated, may hold values from -1.8 to 1.8
Outputs:
- mixed: bfloat16 [3072, 2048], P(('grp', 'sp', 'tp')), parts along dimension 0
The draws below stay inside these ranges and needn't reach their ends.
There are 2 independent parts, one for each index of `grp`. The reference program is written for one: setup_inputs(seed, part) draws one part's arguments, and reference() takes and returns one part's arrays. A program takes and returns all parts, laid end to end along the dimension named above; an argument that names none is the same for every part. Nothing has to cross between parts.
Inputs may be any that keep to these rules, and one draw needn't show every extreme that they name: `route_ids`: among the rows of one device (aligned blocks of 96 tokens) no expert is named more than 30 times, a bound that some block reaches; a token's 2 experts differ.
All inputs are finite; a program needn't handle non-finite values.
Results may differ from the reference program's by a relative error of at most 0.012.
Values may be sent and summed in bfloat16 or wider, within the bound.
A program may use at most 64 MiB of HBM per device.

```python
import math
import jax
import jax.numpy as jnp
import numpy as np
from jax import lax

D = 2048
HEADS = 16
KV_HEADS = 4
HEAD_DIM = 64
ATT_WIDTH = 1024
FF = 3072
TOPK = 2
WINDOW = 128
TOK_DEV = 192
TOK_SUB = 96
TOKENS = 1536
EXPERTS = 8
CAP = 30
DOCS = 4
DOC_MOST = 768
N_TP = 2


def draw_keys(key, part):
    noise = jnp.clip(jax.random.normal(jax.random.fold_in(key, 1), (TOKENS, KV_HEADS, HEAD_DIM), jnp.float32), -6.0, 6.0)
    return noise.reshape(TOKENS, KV_HEADS * HEAD_DIM).astype(jnp.bfloat16)


def draw_queries(key, part):
    noise = jnp.clip(jax.random.normal(jax.random.fold_in(key, 2), (TOKENS, HEADS, HEAD_DIM), jnp.float32), -6.0, 6.0)
    return noise.reshape(TOKENS, HEADS * HEAD_DIM).astype(jnp.bfloat16)


def block_levels(key, dims, cuts, smallest, high):
    gain, own = 1.0, jax.random.fold_in(key, 6)
    for dim, parts in cuts:
        draws = jnp.exp(jax.random.uniform(jax.random.fold_in(own, dim), (parts,), jnp.float32, smallest / len(cuts), high / len(cuts)))
        gain = gain * jnp.repeat(draws, dims[dim] // parts).reshape([-1 if axis == dim else 1 for axis in range(len(dims))])
    return gain


def profile(number_of, total, most, slope):
    weights = [(1 << 20) // math.isqrt(standing ** slope) + 1 for standing in range(2, number_of + 1)]
    surplus, holding = total - most - (number_of - 1), [1] * (number_of - 1)
    while surplus > 0:
        free = [i for i in range(number_of - 1) if holding[i] < most]
        whole, budget = sum([weights[i] for i in free]), surplus
        for i in free:
            extra = min(most - holding[i], max(1, budget * weights[i] // whole), surplus)
            holding[i] = holding[i] + extra
            surplus = surplus - extra
    return np.array([most] + holding)


def uneven(rng, amount, total, most, lean):
    if amount == 2:
        one = jax.random.randint(rng, (), max(1, total - most), min(most, total - 1) + 1)
        return jnp.stack([one, total - one])
    lengths = jnp.asarray(profile(amount, total, most, lean), jnp.int32)
    pairs = (amount - 1) // 2
    source_of, sink = lengths[1:1 + 2 * pairs:2], lengths[2:2 + 2 * pairs:2]
    room = jnp.minimum(source_of - 1, most - sink)
    moved = jax.random.randint(jax.random.fold_in(rng, 1), (pairs,), 0, 1 << 20) % (room + 1)
    lengths = lengths.at[1:1 + 2 * pairs:2].set(source_of - moved).at[2:2 + 2 * pairs:2].set(sink + moved)
    return lengths[jax.random.permutation(jax.random.fold_in(rng, 2), amount)]


def assign_block(rng, own, number, rows, count, top, most, skew):
    sequence = jax.random.permutation(rng, count)
    packed, usual = load_shares(count, rows * top, most, skew, True), load_shares(count, rows * top, most, skew, False)
    places = jnp.arange(count)

    def named(sizes, rotation):
        used = int((sizes > 0).sum())
        fixed = max(1, used // 4)
        moved = fixed + (places - fixed + rotation * (used - fixed)) % max(1, count - fixed)
        return jnp.zeros((count,), jnp.int32).at[sequence[jnp.where(places < fixed, places, moved)]].set(jnp.asarray(sizes, jnp.int32))

    sizes = jnp.where(number % 4 == 0, named(packed, number // 4), named(usual, number - number // 4 - 1))
    mixed = jax.random.permutation(jax.random.fold_in(own, 3), count)
    donor, sink = mixed[0:count // 2 * 2:2], mixed[1:count // 2 * 2:2]
    room = jnp.minimum(sizes[donor] - 1, most - sizes[sink]) // 2
    room = jnp.where((donor == sequence[0]) | (sink == sequence[0]) | (sizes[sink] == 0), 0, jnp.maximum(room, 0))
    moved = jax.random.randint(jax.random.fold_in(own, 4), (count // 2,), 0, 1 << 20) % (room + 1)
    sizes = sizes.at[donor].add(-moved).at[sink].add(moved)
    labels = jnp.searchsorted(jnp.cumsum(sizes), jnp.arange(rows * top), side="right").astype(jnp.int32)
    grid = labels.reshape(top, rows).T
    grid = grid[jax.random.permutation(jax.random.fold_in(own, 1), rows)]
    rotation = jax.random.randint(jax.random.fold_in(own, 2), (rows, 1), 0, top)
    return jnp.take_along_axis(grid, (jnp.arange(top)[None, :] + rotation) % top, axis=1)


def load_shares(amount, total, limit, skew, full):
    weights = [(1 << 20) // math.isqrt(grade ** skew) + 1 for grade in range(1, amount + 1)]
    largest = limit if full else min(limit, max(-(-total // amount), total * weights[0] // sum(weights)))
    least = 1 if total - largest >= amount - 1 else 0
    given, rest = [largest] + [least] * (amount - 1), total - largest - least * (amount - 1)
    while rest > 0:
        free = [i for i in range(1, amount) if given[i] < largest] or [i for i in range(1, amount) if given[i] < limit]
        mass, budget = sum([weights[i] for i in free]), rest
        for i in free:
            extra = min(limit - given[i], max(1, budget * weights[i] // mass), rest)
            given[i] = given[i] + extra
            rest = rest - extra
    return np.array(given)


def normal_values(own_key, extent, spread, most, shards=(), held_as=jnp.bfloat16):
    values = jax.random.normal(own_key, extent, jnp.float32) * spread
    if len(shards) > 0:
        values = block_levels(own_key, extent, shards, -0.22, 0.18) * values
    return jnp.clip(values, min=-most, max=most).astype(held_as)


def setup_inputs(seed: int = 0, part: int = 0) -> dict:
    seeds = jax.random.split(jax.random.key(seed), 17)
    part_keys = jax.random.split(jax.random.fold_in(seeds[16], part), 17)
    resid = normal_values(part_keys[0], (TOKENS, D), 1.0, 6.0, ((0, 16),))
    queries = draw_queries(jax.random.fold_in(jax.random.fold_in(seeds[16], part), 71), part)
    keys = draw_keys(jax.random.fold_in(jax.random.fold_in(seeds[16], part), 71), part)
    values = normal_values(part_keys[3], (TOKENS, KV_HEADS * HEAD_DIM), 1.0, 6.0, ((0, 8), (1, 2)))
    doc_ids = jnp.searchsorted(jnp.cumsum(uneven(part_keys[4], DOCS, TOKENS, DOC_MOST, 2)), jnp.arange(TOKENS), side="right").astype(jnp.int32)
    sink_logits = jnp.clip(2.0 + 4.0 * jax.random.uniform(seeds[5], (HEADS,), jnp.float32) ** block_levels(seeds[5], (HEADS,), ((0, 2),), -0.2, 0.2), 2.0, 6.0)
    out_proj = normal_values(seeds[6], (ATT_WIDTH, D), (HEAD_DIM // 4) ** -0.5, 1.5, ((0, 2),))
    norm1_gain = jnp.clip(1.0 + 0.18 * jax.random.normal(seeds[7], (D,), jnp.float32), 0.1, 1.9)
    norm1_bias = normal_values(seeds[8], (D,), 0.3, 1.8, (), jnp.float32)
    route_ids_keys = jax.random.split(jax.random.fold_in(part_keys[9], 1), TOKENS // TOK_SUB)
    route_ids_turns = jax.random.permutation(jax.random.fold_in(part_keys[9], 3), TOKENS // TOK_SUB)
    route_ids = jax.vmap(lambda own, number: assign_block(jax.random.fold_in(part_keys[9], 2), own, number, TOK_SUB, EXPERTS, TOPK, CAP, 1))(route_ids_keys, route_ids_turns).reshape((TOKENS, TOPK))
    route_weights = jnp.clip(0.25 + 0.75 * jax.random.uniform(part_keys[10], (TOKENS, TOPK), jnp.float32) ** block_levels(part_keys[10], (TOKENS, TOPK), ((0, 16),), -0.2, 0.2), 0.25, 1.0)
    expert_gate = normal_values(seeds[11], (EXPERTS, D, FF), D ** -0.5, 0.125, ((0, 8), (2, 2)))
    expert_up = normal_values(seeds[12], (EXPERTS, D, FF), D ** -0.5, 0.125, ((0, 8), (2, 2)))
    expert_down = normal_values(seeds[13], (EXPERTS, FF, D), FF ** -0.5, 0.109375, ((0, 8), (1, 2)))
    norm2_gain = jnp.clip(1.0 + 0.18 * jax.random.normal(seeds[14], (D,), jnp.float32), 0.1, 1.9)
    norm2_bias = normal_values(seeds[15], (D,), 0.3, 1.8, (), jnp.float32)
    return {"resid": resid, "queries": queries, "keys": keys, "values": values, "doc_ids": doc_ids, "sink_logits": sink_logits, "out_proj": out_proj, "norm1_gain": norm1_gain, "norm1_bias": norm1_bias, "route_ids": route_ids, "route_weights": route_weights, "expert_gate": expert_gate, "expert_up": expert_up, "expert_down": expert_down, "norm2_gain": norm2_gain, "norm2_bias": norm2_bias}


norm_epsilon = 1e-05
residual_scale = 1.4142135623730951
masked_score = -1e+30

def layer_norm(values, gain_vec, bias_vec):
    mean_val = lax.optimization_barrier(jnp.mean(values, -1, keepdims=True))
    centred = values - mean_val
    variance = lax.optimization_barrier(jnp.mean(centred * centred, -1, keepdims=True))
    return centred * lax.rsqrt(variance + norm_epsilon) * gain_vec + bias_vec

def attention(queries, keys, values, doc_ids, sink_logits):
    groups = HEADS // KV_HEADS
    block = TOK_DEV
    nblocks = TOKENS // block
    reach = block + 2 * WINDOW
    pad_keys = jnp.pad(keys.reshape(TOKENS, KV_HEADS, HEAD_DIM), ((WINDOW, WINDOW), (0, 0), (0, 0)))
    pad_values = jnp.pad(values.reshape(TOKENS, KV_HEADS, HEAD_DIM), ((WINDOW, WINDOW), (0, 0), (0, 0)))
    pad_docs = jnp.pad(doc_ids.astype(jnp.int32), (WINDOW, WINDOW))
    sink_table = sink_logits.astype(jnp.float32).reshape(KV_HEADS, groups, 1, 1)

    def one_block(index):
        start = index * block
        query_blk = lax.dynamic_slice_in_dim(queries, start, block, 0).reshape(block, KV_HEADS, groups, HEAD_DIM)
        key_blk = lax.dynamic_slice_in_dim(pad_keys, start, reach, 0)
        value_blk = lax.dynamic_slice_in_dim(pad_values, start, reach, 0)
        query_docs = lax.dynamic_slice_in_dim(doc_ids.astype(jnp.int32), start, block, 0)
        key_docs = lax.dynamic_slice_in_dim(pad_docs, start, reach, 0)
        query_pos = start + jnp.arange(block, dtype=jnp.int32)
        key_pos = start - WINDOW + jnp.arange(reach, dtype=jnp.int32)
        allowed = (key_pos[None, :] >= 0) & (key_pos[None, :] < TOKENS)
        allowed = allowed & (jnp.abs(query_pos[:, None] - key_pos[None, :]) <= WINDOW)
        allowed = allowed & (query_docs[:, None] == key_docs[None, :])
        scores = jnp.einsum('qkgd,jkd->kgqj', query_blk.astype(jnp.float32), key_blk.astype(jnp.float32))
        scores = jnp.where(allowed, scores * HEAD_DIM ** (-0.5), masked_score)
        top_score = jnp.maximum(lax.optimization_barrier(jnp.max(scores, -1, keepdims=True)), sink_table)
        raised = jnp.where(allowed, jnp.exp(scores - top_score), 0.0)
        denominator = jnp.exp(sink_table - top_score) + lax.optimization_barrier(jnp.sum(raised, -1, keepdims=True))
        weights = (raised / denominator).astype(jnp.bfloat16)
        result = jnp.einsum('kgqj,jkd->qkgd', weights.astype(jnp.float32), value_blk.astype(jnp.float32))
        return result.astype(jnp.bfloat16).reshape(block, HEADS * HEAD_DIM)
    blocks = lax.map(one_block, jnp.arange(nblocks, dtype=jnp.int32))
    return blocks.reshape(TOKENS, HEADS * HEAD_DIM)

def experts_part(normed, route_ids, route_weights, expert_gate, expert_up, expert_down):
    nblocks = TOKENS // TOK_SUB
    slot_count = nblocks * CAP
    flat_ids = route_ids.reshape(nblocks, TOK_SUB * TOPK).astype(jnp.int32)
    one_hot = (flat_ids[:, :, None] == jnp.arange(EXPERTS, dtype=jnp.int32)[None, None, :]).astype(jnp.int32)
    ranks = (jnp.cumsum(one_hot, axis=1) - 1).astype(jnp.int32)
    slot_rank = lax.optimization_barrier(jnp.sum(ranks * one_hot, axis=-1)).astype(jnp.int32)
    block_ids = jnp.arange(nblocks, dtype=jnp.int32)[:, None]
    targets = (flat_ids * slot_count + block_ids * CAP + slot_rank).reshape(-1).astype(jnp.int32)
    owners = (block_ids * TOK_SUB + jnp.arange(TOK_SUB * TOPK, dtype=jnp.int32)[None, :] // TOPK).reshape(-1).astype(jnp.int32)
    token_table = jnp.full((EXPERTS * slot_count,), TOKENS, jnp.int32).at[targets].set(owners).reshape(EXPERTS, slot_count)
    weight_table = jnp.zeros((EXPERTS * slot_count,), jnp.float32).at[targets].set(route_weights.reshape(-1).astype(jnp.float32)).reshape(EXPERTS, slot_count)
    padded = jnp.concatenate([normed, jnp.zeros((1, D), normed.dtype)], 0)
    hidden_cols = FF // N_TP

    def one_expert(total, inputs):
        gate_weight, up_weight, down_weight, token_rows, row_weights = inputs
        row_block = jnp.take(padded, token_rows, axis=0)
        gate_act = jnp.dot(row_block, gate_weight, preferred_element_type=jnp.float32)
        up_act = jnp.dot(row_block, up_weight, preferred_element_type=jnp.float32)
        hidden = (jax.nn.silu(gate_act) * up_act).astype(jnp.bfloat16)
        summed = jnp.zeros((slot_count, D), jnp.float32)
        for member in range(N_TP):
            piece_out = jnp.dot(hidden[:, member * hidden_cols:(member + 1) * hidden_cols], down_weight[member * hidden_cols:(member + 1) * hidden_cols], preferred_element_type=jnp.float32)
            summed = summed + lax.optimization_barrier(piece_out.astype(jnp.bfloat16)).astype(jnp.float32)
        expert_out = lax.optimization_barrier(summed.astype(jnp.bfloat16)).astype(jnp.float32)
        return (total.at[token_rows].add(row_weights[:, None] * expert_out), None)
    total, _ = lax.scan(one_expert, jnp.zeros((TOKENS + 1, D), jnp.float32), (expert_gate, expert_up, expert_down, token_table, weight_table))
    return total[:TOKENS]

def reference(resid, queries, keys, values, doc_ids, sink_logits, out_proj, norm1_gain, norm1_bias, route_ids, route_weights, expert_gate, expert_up, expert_down, norm2_gain, norm2_bias):
    attended = attention(queries, keys, values, doc_ids, sink_logits)
    head_cols = ATT_WIDTH // N_TP
    projected = jnp.zeros((TOKENS, D), jnp.float32)
    for member in range(N_TP):
        piece_out = jnp.dot(attended[:, member * head_cols:(member + 1) * head_cols], out_proj[member * head_cols:(member + 1) * head_cols], preferred_element_type=jnp.float32)
        projected = projected + lax.optimization_barrier(piece_out.astype(jnp.bfloat16)).astype(jnp.float32)
    projected = lax.optimization_barrier(projected.astype(jnp.bfloat16)).astype(jnp.float32)
    pre_norm = residual_scale * resid.astype(jnp.float32) + projected
    normed = layer_norm(pre_norm, norm1_gain, norm1_bias).astype(jnp.bfloat16)
    moe_sum = experts_part(normed, route_ids, route_weights, expert_gate, expert_up, expert_down)
    pre_final = residual_scale * normed.astype(jnp.float32) + moe_sum
    return layer_norm(pre_final, norm2_gain, norm2_bias).astype(jnp.bfloat16)
```

```python
import functools

import jax
import jax.numpy as jnp
from jax import lax
from jax.experimental import pallas as pl
from jax.experimental.pallas import tpu as pltpu
from jax.sharding import PartitionSpec as P

HEAD_DIM = 64
WINDOW = 128
MESH = pl.DeviceIdType.MESH


norm_epsilon = 1e-05
residual_scale = 1.4142135623730951
masked_score = -1e30


def with_halo(cells, sides, width):
    for axis, dim in sides:
        count = lax.axis_size(axis)
        ends = count - 1
        head = lax.slice_in_dim(cells, 0, width, axis=dim)
        tail = lax.slice_in_dim(cells, cells.shape[dim] - width, cells.shape[dim], axis=dim)
        cells = jnp.concatenate(
            [
                lax.ppermute(tail, axis, [(i, (i + 1) % count) for i in range(ends)]),
                cells,
                lax.ppermute(head, axis, [((i + 1) % count, i) for i in range(ends)]),
            ],
            axis=dim,
        )
    return cells


def layer_norm(values, gain_vec, bias_vec):
    mean_val = jnp.mean(values, -1, keepdims=True)
    centred = values - mean_val
    variance = jnp.mean(centred * centred, -1, keepdims=True)
    return centred * lax.rsqrt(variance + norm_epsilon) * gain_vec + bias_vec


def step_partner(step, sp_pos, count, back):
    chip, core = sp_pos // 2, sp_pos % 2
    half = count // 4
    side, place = chip // half, chip % half
    pair, flip = step // 2, step % 2
    if pair == 0:
        turn, cross = 0, False
    elif pair <= half:
        turn, cross = pair - 1, True
    else:
        turn, cross = pair - half, False
    target_side = 1 - side if cross else side
    move = half - turn if back else turn
    target = target_side * half + (place + move) % half
    return target * 2 + (core + flip) % 2


def moe_kernel(
    experts,
    tps,
    chunk,
    normed_ref,
    ids_ref,
    rw_ref,
    gain_ref,
    bias_ref,
    gate_hbm,
    up_hbm,
    down_hbm,
    out_ref,
    outgoing,
    rows,
    gate_w,
    up_w,
    down_w,
    hidden,
    part,
    peer,
    summed,
    returned,
    w_sem,
    disp_send,
    disp_recv,
    fwd_send,
    fwd_recv,
    part_send,
    part_recv,
    ret_send,
    ret_recv,
):
    me, t = lax.axis_index("sp"), lax.axis_index("tp")
    _, capacity, width = outgoing.shape
    toks = normed_ref.shape[0]
    weight_copies = [
        pltpu.make_async_copy(gate_hbm.at[0], gate_w, w_sem.at[0]),
        pltpu.make_async_copy(up_hbm.at[0], up_w, w_sem.at[1]),
        pltpu.make_async_copy(down_hbm.at[0], down_w, w_sem.at[2]),
    ]
    for copy in weight_copies:
        copy.start()

    barrier = pltpu.get_barrier_semaphore()
    for d in range(1, experts):
        pl.semaphore_signal(
            barrier, inc=1, device_id={"sp": (me + d) % experts}, device_id_type=MESH
        )
    for d in range(1, tps):
        pl.semaphore_signal(barrier, inc=1, device_id={"tp": (t + d) % tps}, device_id_type=MESH)

    lanes = experts * capacity
    ids = ids_ref[...]
    wide = max(experts, 128)
    expert_iota = lax.broadcasted_iota(jnp.int32, (toks, wide), 1)
    lower = (
        lax.broadcasted_iota(jnp.int32, (toks, toks), 0)
        > lax.broadcasted_iota(jnp.int32, (toks, toks), 1)
    ).astype(jnp.float32).astype(jnp.bfloat16)
    before = jnp.zeros((1, wide), jnp.float32)
    slot_iota = lax.broadcasted_iota(jnp.int32, (toks, lanes), 1)
    assign = jnp.zeros((toks, lanes), jnp.float32)
    combine = jnp.zeros((toks, lanes), jnp.float32)
    for k in range(ids.shape[1]):
        own = ids[:, k : k + 1]
        hot = (own == expert_iota).astype(jnp.float32)
        rank = before + jnp.dot(lower, hot.astype(jnp.bfloat16), preferred_element_type=jnp.float32)
        rank = jnp.sum(rank * hot, axis=1, keepdims=True).astype(jnp.int32)
        before = before + jnp.sum(hot, axis=0, keepdims=True)
        match = (own * capacity + rank == slot_iota).astype(jnp.float32)
        assign = assign + match
        combine = combine + match * rw_ref[:, k : k + 1]
    spread = lax.dot_general(
        assign.astype(jnp.bfloat16),
        normed_ref[...],
        (((0,), (0,)), ((), ())),
        preferred_element_type=jnp.float32,
    )
    outgoing[...] = spread.astype(jnp.bfloat16).reshape(experts, capacity, width)
    rows[0, t] = outgoing[me]

    pl.semaphore_wait(barrier, experts - 1 + tps - 1)

    def dispatch(step):
        dst = step_partner(step, me, experts, False)
        return pltpu.make_async_remote_copy(
            src_ref=outgoing.at[dst],
            dst_ref=rows.at[step, t],
            send_sem=disp_send.at[step],
            recv_sem=disp_recv.at[step],
            device_id={"sp": dst},
            device_id_type=MESH,
        )

    def forward(step, d):
        dst = (t + d) % tps
        return pltpu.make_async_remote_copy(
            src_ref=rows.at[step, t],
            dst_ref=rows.at[step, t],
            send_sem=fwd_send.at[step, d],
            recv_sem=fwd_recv.at[step, d],
            device_id={"tp": dst},
            device_id_type=MESH,
        )

    def share(step, d):
        dst = (t + d) % tps
        return pltpu.make_async_remote_copy(
            src_ref=part.at[step, dst],
            dst_ref=peer.at[step, d],
            send_sem=part_send.at[step, d],
            recv_sem=part_recv.at[step, d],
            device_id={"tp": dst},
            device_id_type=MESH,
        )

    def give_back(step):
        dst = step_partner(step, me, experts, True)
        return pltpu.make_async_remote_copy(
            src_ref=summed.at[step],
            dst_ref=returned.at[me],
            send_sem=ret_send.at[step],
            recv_sem=ret_recv.at[step],
            device_id={"sp": dst},
            device_id_type=MESH,
        )

    for step in range(1, experts):
        dispatch(step).start()

    def send_on(step):
        if step > 0:
            dispatch(step).wait_recv()
        for d in range(1, tps):
            forward(step, d).start()

    def finish(step):
        total = part[step, t].astype(jnp.float32)
        for d in range(1, tps):
            share(step, d).wait_recv()
            total = total + peer[step, d].astype(jnp.float32)
        if step == 0:
            returned[me] = total.astype(jnp.bfloat16)
        else:
            summed[step] = total.astype(jnp.bfloat16)
            give_back(step).start()

    tile = 256
    hidden_width = gate_w.shape[1]
    m = chunk * tps * capacity
    chunks = experts // chunk

    for c in range(chunks):
        k0, k1 = c * chunk, (c + 1) * chunk
        for step in range(k0, k1):
            send_on(step)
        for step in range(k0, k1):
            for d in range(1, tps):
                forward(step, d).wait_recv()
        if c == 0:
            weight_copies[0].wait()
            weight_copies[1].wait()

        def up_tile(i, carry):
            cols = pl.ds(pl.multiple_of(i * tile, tile), tile)
            block = rows[k0:k1].reshape(m, width)
            gate = jnp.dot(block, gate_w[:, cols], preferred_element_type=jnp.float32)
            up = jnp.dot(block, up_w[:, cols], preferred_element_type=jnp.float32)
            hidden[:, cols] = (gate / (1.0 + jnp.exp(-gate)) * up).astype(jnp.bfloat16)
            return carry

        lax.fori_loop(0, hidden_width // tile, up_tile, 0)
        if c == 0:
            weight_copies[2].wait()

        def down_tile(i, carry):
            cols = pl.ds(pl.multiple_of(i * tile, tile), tile)
            result = jnp.dot(hidden[...], down_w[:, cols], preferred_element_type=jnp.float32)
            part[k0:k1, :, :, cols] = result.astype(jnp.bfloat16).reshape(
                chunk, tps, capacity, tile
            )
            return carry

        lax.fori_loop(0, width // tile, down_tile, 0)
        for step in range(k0, k1):
            for d in range(1, tps):
                share(step, d).start()
        if c > 0:
            for step in range(k0 - chunk, k0):
                finish(step)
    for step in range(experts - chunk, experts):
        finish(step)
    for step in range(1, experts):
        src = step_partner(step, me, experts, False)
        pltpu.make_async_remote_copy(
            src_ref=summed.at[step],
            dst_ref=returned.at[src],
            send_sem=ret_send.at[step],
            recv_sem=ret_recv.at[step],
            device_id={"sp": src},
            device_id_type=MESH,
        ).wait_recv()

    back = returned[...].reshape(lanes, width)
    high = combine.astype(jnp.bfloat16)
    low = (combine - high.astype(jnp.float32)).astype(jnp.bfloat16)
    moe_sum = jnp.dot(high, back, preferred_element_type=jnp.float32)
    moe_sum = moe_sum + jnp.dot(low, back, preferred_element_type=jnp.float32)
    pre_final = residual_scale * normed_ref[...].astype(jnp.float32) + moe_sum
    out_ref[...] = layer_norm(pre_final, gain_ref[...], bias_ref[...]).astype(jnp.bfloat16)

    for step in range(experts):
        if step > 0:
            dispatch(step).wait_send()
            give_back(step).wait_send()
        for d in range(1, tps):
            forward(step, d).wait_send()
            share(step, d).wait_send()


def run_moe(normed, route_ids, route_weights, gate, up, down, gain, bias):
    experts, tps = lax.axis_size("sp"), lax.axis_size("tp")
    toks, width = normed.shape
    need = 5 * toks // (2 * experts)
    capacity = -(-need // 16) * 16
    chunk = experts // 2
    hidden_width = gate.shape[2]
    vmem = pl.BlockSpec(memory_space=pltpu.VMEM)
    hbm = pl.BlockSpec(memory_space=pl.ANY)
    bf16 = jnp.bfloat16
    dma = pltpu.SemaphoreType.DMA
    return pl.pallas_call(
        functools.partial(moe_kernel, experts, tps, chunk),
        out_shape=jax.ShapeDtypeStruct((toks, width), bf16),
        in_specs=[vmem] * 5 + [hbm] * 3,
        out_specs=vmem,
        scratch_shapes=[
            pltpu.VMEM((experts, capacity, width), bf16),
            pltpu.VMEM((experts, tps, capacity, width), bf16),
            pltpu.VMEM((width, hidden_width), bf16),
            pltpu.VMEM((width, hidden_width), bf16),
            pltpu.VMEM((hidden_width, width), bf16),
            pltpu.VMEM((chunk * tps * capacity, hidden_width), bf16),
            pltpu.VMEM((experts, tps, capacity, width), bf16),
            pltpu.VMEM((experts, tps, capacity, width), bf16),
            pltpu.VMEM((experts, capacity, width), bf16),
            pltpu.VMEM((experts, capacity, width), bf16),
            dma((3,)),
            dma((experts,)),
            dma((experts,)),
            dma((experts, tps)),
            dma((experts, tps)),
            dma((experts, tps)),
            dma((experts, tps)),
            dma((experts,)),
            dma((experts,)),
        ],
        compiler_params=pltpu.CompilerParams(
            collective_id=0, has_side_effects=True, vmem_limit_bytes=60 * 1024 * 1024
        ),
    )(normed, route_ids, route_weights, gain[None, :], bias[None, :], gate, up, down)


def per_device(
    resid,
    queries,
    keys,
    values,
    doc_ids,
    sink_logits,
    out_proj,
    norm1_gain,
    norm1_bias,
    route_ids,
    route_weights,
    expert_gate,
    expert_up,
    expert_down,
    norm2_gain,
    norm2_bias,
):
    tok_dev = queries.shape[0]
    local_kv = keys.shape[1] // HEAD_DIM
    local_heads = queries.shape[1] // HEAD_DIM
    groups = local_heads // local_kv
    reach = tok_dev + 2 * WINDOW
    padded_keys, padded_values, padded_docs = (
        with_halo(keys, (("sp", 0),), WINDOW),
        with_halo(values, (("sp", 0),), WINDOW),
        with_halo(doc_ids, (("sp", 0),), WINDOW),
    )
    offset = lax.axis_index("sp") * tok_dev
    seq_total = lax.axis_size("sp") * tok_dev
    query_pos = offset + jnp.arange(tok_dev, dtype=jnp.int32)
    key_pos = offset - WINDOW + jnp.arange(reach, dtype=jnp.int32)
    allowed = (key_pos[None, :] >= 0) & (key_pos[None, :] < seq_total)
    allowed = allowed & (jnp.abs(query_pos[:, None] - key_pos[None, :]) <= WINDOW)
    allowed = allowed & (doc_ids[:, None] == padded_docs[None, :])
    query_heads = queries.reshape(tok_dev, local_kv, groups, HEAD_DIM)
    key_heads = padded_keys.reshape(reach, local_kv, HEAD_DIM)
    value_heads = padded_values.reshape(reach, local_kv, HEAD_DIM)
    sink_local = sink_logits.reshape(local_kv, groups, 1, 1)
    scores = jnp.einsum(
        "qkgd,jkd->kgqj", query_heads, key_heads, preferred_element_type=jnp.float32
    )
    scores = jnp.where(allowed, scores * HEAD_DIM ** (-0.5), masked_score)
    top_score = jnp.maximum(jnp.max(scores, -1, keepdims=True), sink_local)
    raised = jnp.where(allowed, jnp.exp(scores - top_score), 0.0)
    denominator = jnp.exp(sink_local - top_score) + jnp.sum(raised, -1, keepdims=True)
    weights = (raised / denominator).astype(jnp.bfloat16)
    attended = jnp.einsum(
        "kgqj,jkd->qkgd", weights, value_heads, preferred_element_type=jnp.float32
    )
    attended = attended.astype(jnp.bfloat16).reshape(tok_dev, local_heads * HEAD_DIM)
    projected = lax.psum_scatter(
        jnp.dot(attended, out_proj, preferred_element_type=jnp.float32).astype(jnp.bfloat16),
        "tp",
        scatter_dimension=0,
        tiled=True,
    )
    pre_norm = residual_scale * resid.astype(jnp.float32) + projected.astype(jnp.float32)
    normed = layer_norm(pre_norm, norm1_gain, norm1_bias).astype(jnp.bfloat16)
    return run_moe(
        normed, route_ids, route_weights, expert_gate, expert_up, expert_down, norm2_gain, norm2_bias
    )


def solution(mesh):
    return jax.shard_map(
        per_device,
        mesh=mesh,
        in_specs=(
            P(("grp", "sp", "tp"), None),
            P(("grp", "sp"), "tp"),
            P(("grp", "sp"), "tp"),
            P(("grp", "sp"), "tp"),
            P(("grp", "sp")),
            P("tp"),
            P("tp", None),
            P(),
            P(),
            P(("grp", "sp", "tp"), None),
            P(("grp", "sp", "tp"), None),
            P("sp", None, "tp"),
            P("sp", None, "tp"),
            P("sp", "tp", None),
            P(),
            P(),
        ),
        out_specs=P(("grp", "sp", "tp"), None),
        check_vma=False,
    )
```

```python
import functools

import jax
import jax.numpy as jnp
from jax import lax
from jax.experimental import pallas as pl
from jax.experimental.pallas import tpu as pltpu
from jax.sharding import PartitionSpec as P

HEAD_DIM = 64
WINDOW = 128
MESH = pl.DeviceIdType.MESH
CHUNKS = 2


norm_epsilon = 1e-05
residual_scale = 1.4142135623730951
masked_score = -1e30


def layer_norm(values, gain_vec, bias_vec):
    mean_val = jnp.mean(values, -1, keepdims=True)
    centred = values - mean_val
    variance = jnp.mean(centred * centred, -1, keepdims=True)
    return centred * lax.rsqrt(variance + norm_epsilon) * gain_vec + bias_vec


def step_partner(step, sp_pos, count, back):
    chip, core = sp_pos // 2, sp_pos % 2
    half = count // 4
    side, place = chip // half, chip % half
    pair, flip = step // 2, step % 2
    if pair == 0:
        turn, cross = 0, False
    elif pair <= half:
        turn, cross = pair - 1, True
    else:
        turn, cross = pair - half, False
    target_side = 1 - side if cross else side
    move = half - turn if back else turn
    target = target_side * half + (place + move) % half
    return target * 2 + (core + flip) % 2


def head_copy(d, t, tps, head_part, head_peer, head_send, head_recv):
    return pltpu.make_async_remote_copy(
        src_ref=head_part.at[d],
        dst_ref=head_peer.at[d],
        send_sem=head_send.at[d],
        recv_sem=head_recv.at[d],
        device_id={"tp": (t + d) % tps},
        device_id_type=MESH,
    )


def attend(
    count,
    tps,
    queries_ref,
    keys_ref,
    values_ref,
    docs_ref,
    sink_ref,
    proj_w,
    key_pad,
    value_pad,
    doc_pad,
    attended,
    head_part,
    head_peer,
    halo_send,
    halo_recv,
    head_send,
    head_recv,
    barrier,
    first_copies,
):
    me, t = lax.axis_index("sp"), lax.axis_index("tp")
    tok_dev, tok_sub = queries_ref.shape[0], attended.shape[0]
    local_kv = keys_ref.shape[1] // HEAD_DIM
    heads = queries_ref.shape[1] // HEAD_DIM
    groups = heads // local_kv
    reach = -(-(tok_sub + 2 * WINDOW) // 128) * 128
    end = WINDOW + tok_dev
    rest = key_pad.shape[0] - end - WINDOW
    for pad, own in ((key_pad, keys_ref), (value_pad, values_ref), (doc_pad, docs_ref)):
        pad[WINDOW:end] = own[...]
        if rest:
            pad[end + WINDOW :] = jnp.zeros((rest, pad.shape[1]), pad.dtype)
    pl.semaphore_wait(barrier, count - 1 + tps - 1)
    copies = []
    for i, (pad, own) in enumerate(
        ((key_pad, keys_ref), (value_pad, values_ref), (doc_pad, docs_ref))
    ):
        for side in range(2):
            start, place = (tok_dev - WINDOW, 0) if side == 0 else (0, end)
            copies.append(
                pltpu.make_async_remote_copy(
                    src_ref=own.at[pl.ds(start, WINDOW)],
                    dst_ref=pad.at[pl.ds(place, WINDOW)],
                    send_sem=halo_send.at[2 * i + side],
                    recv_sem=halo_recv.at[2 * i + side],
                    device_id={"sp": (me + 1) % count if side == 0 else (me + count - 1) % count},
                    device_id_type=MESH,
                )
            )
    for copy in copies:
        copy.start()
    for copy in copies:
        copy.wait_recv()

    for d in list(range(1, tps)) + [0]:
        base = pl.multiple_of((t + d) % tps * tok_sub, 16)
        key_block = key_pad[pl.ds(base, reach), :].astype(jnp.float32)
        value_block = value_pad[pl.ds(base, reach), :].astype(jnp.float32)
        key_docs = jnp.transpose(doc_pad[pl.ds(base, reach), :])[0:1, :]
        query_docs = docs_ref[pl.ds(base, tok_sub), 0:1]
        row = lax.broadcasted_iota(jnp.int32, (tok_sub, reach), 0)
        col = lax.broadcasted_iota(jnp.int32, (tok_sub, reach), 1)
        position = me * tok_dev + base - WINDOW + col
        allowed = (position >= 0) & (position < count * tok_dev)
        allowed = allowed & (col >= row) & (col <= row + 2 * WINDOW)
        allowed = allowed & (query_docs == key_docs)
        blank = jnp.zeros((reach, HEAD_DIM), jnp.float32)
        for g in range(local_kv):
            span = slice(g * HEAD_DIM, (g + 1) * HEAD_DIM)
            sides = []
            for block in (key_block, value_block):
                piece = block[:, span]
                sides.append(
                    [
                        jnp.concatenate([piece, blank], 1).astype(jnp.bfloat16),
                        jnp.concatenate([blank, piece], 1).astype(jnp.bfloat16),
                    ]
                )
            for pair in range(groups // 2):
                lane = (g * groups + 2 * pair) * HEAD_DIM
                query = queries_ref[pl.ds(base, tok_sub), lane : lane + 2 * HEAD_DIM]
                result = jnp.zeros((tok_sub, 2 * HEAD_DIM), jnp.float32)
                for parity in range(2):
                    head = g * groups + 2 * pair + parity
                    sink = sink_ref[:, head : head + 1]
                    scores = lax.dot_general(
                        query,
                        sides[0][parity],
                        (((1,), (1,)), ((), ())),
                        preferred_element_type=jnp.float32,
                    )
                    scores = jnp.where(allowed, scores * HEAD_DIM ** (-0.5), masked_score)
                    top = jnp.maximum(jnp.max(scores, -1, keepdims=True), sink)
                    raised = jnp.where(allowed, jnp.exp(scores - top), 0.0)
                    total = jnp.exp(sink - top) + jnp.sum(raised, -1, keepdims=True)
                    weights = (raised / total).astype(jnp.bfloat16)
                    result = result + jnp.dot(
                        weights, sides[1][parity], preferred_element_type=jnp.float32
                    )
                attended[:, lane : lane + 2 * HEAD_DIM] = result.astype(jnp.bfloat16)
        if d == 1 or tps == 1:
            for copy in first_copies:
                copy.wait()
        tile = 512
        width = proj_w.shape[1]

        def project(i, carry):
            cols = pl.ds(pl.multiple_of(i * tile, tile), tile)
            head_part[d, :, cols] = jnp.dot(
                attended[...], proj_w[:, cols], preferred_element_type=jnp.float32
            ).astype(jnp.bfloat16)
            return carry

        lax.fori_loop(0, width // tile, project, 0)
        if d:
            head_copy(d, t, tps, head_part, head_peer, head_send, head_recv).start()
    for copy in copies:
        copy.wait_send()


def layer_kernel(
    experts,
    tps,
    chunk,
    queries_ref,
    keys_ref,
    values_ref,
    docs_ref,
    sink_ref,
    gain1_ref,
    bias1_ref,
    ids_ref,
    rw_ref,
    gain_ref,
    bias_ref,
    resid_hbm,
    proj_hbm,
    gate_hbm,
    up_hbm,
    down_hbm,
    out_ref,
    resid_ref,
    proj_w,
    key_pad,
    value_pad,
    doc_pad,
    attended,
    head_part,
    head_peer,
    normed_ref,
    outgoing,
    rows,
    gate_w,
    up_w,
    down_w,
    hidden,
    part,
    peer,
    summed,
    returned,
    w_sem,
    disp_send,
    disp_recv,
    fwd_send,
    fwd_recv,
    part_send,
    part_recv,
    ret_send,
    ret_recv,
    halo_send,
    halo_recv,
    head_send,
    head_recv,
):
    me, t = lax.axis_index("sp"), lax.axis_index("tp")
    _, capacity, width = outgoing.shape
    toks = normed_ref.shape[0]
    first_copies = [
        pltpu.make_async_copy(resid_hbm, resid_ref, w_sem.at[3]),
        pltpu.make_async_copy(proj_hbm, proj_w, w_sem.at[4]),
    ]
    for copy in first_copies:
        copy.start()
    weight_copies = [
        pltpu.make_async_copy(gate_hbm.at[0], gate_w, w_sem.at[0]),
        pltpu.make_async_copy(up_hbm.at[0], up_w, w_sem.at[1]),
        pltpu.make_async_copy(down_hbm.at[0], down_w, w_sem.at[2]),
    ]
    for copy in weight_copies:
        copy.start()

    barrier = pltpu.get_barrier_semaphore()
    for d in range(1, experts):
        pl.semaphore_signal(
            barrier, inc=1, device_id={"sp": (me + d) % experts}, device_id_type=MESH
        )
    for d in range(1, tps):
        pl.semaphore_signal(barrier, inc=1, device_id={"tp": (t + d) % tps}, device_id_type=MESH)

    attend(
        experts,
        tps,
        queries_ref,
        keys_ref,
        values_ref,
        docs_ref,
        sink_ref,
        proj_w,
        key_pad,
        value_pad,
        doc_pad,
        attended,
        head_part,
        head_peer,
        halo_send,
        halo_recv,
        head_send,
        head_recv,
        barrier,
        first_copies,
    )
    lanes = experts * capacity
    ids = ids_ref[...]
    wide = max(experts, 128)
    expert_iota = lax.broadcasted_iota(jnp.int32, (toks, wide), 1)
    lower = (
        lax.broadcasted_iota(jnp.int32, (toks, toks), 0)
        > lax.broadcasted_iota(jnp.int32, (toks, toks), 1)
    ).astype(jnp.float32).astype(jnp.bfloat16)
    before = jnp.zeros((1, wide), jnp.float32)
    slot_iota = lax.broadcasted_iota(jnp.int32, (toks, lanes), 1)
    assign = jnp.zeros((toks, lanes), jnp.float32)
    combine = jnp.zeros((toks, lanes), jnp.float32)
    for k in range(ids.shape[1]):
        own = ids[:, k : k + 1]
        hot = (own == expert_iota).astype(jnp.float32)
        rank = before + jnp.dot(lower, hot.astype(jnp.bfloat16), preferred_element_type=jnp.float32)
        rank = jnp.sum(rank * hot, axis=1, keepdims=True).astype(jnp.int32)
        before = before + jnp.sum(hot, axis=0, keepdims=True)
        match = (own * capacity + rank == slot_iota).astype(jnp.float32)
        assign = assign + match
        combine = combine + match * rw_ref[:, k : k + 1]
    projected = head_part[0].astype(jnp.float32)
    for d in range(1, tps):
        head_copy(d, t, tps, head_part, head_peer, head_send, head_recv).wait_recv()
        projected = projected + head_peer[d].astype(jnp.float32)
    projected = projected.astype(jnp.bfloat16).astype(jnp.float32)
    pre_norm = residual_scale * resid_ref[...].astype(jnp.float32) + projected
    normed_ref[...] = layer_norm(pre_norm, gain1_ref[...], bias1_ref[...]).astype(jnp.bfloat16)
    spread = lax.dot_general(
        assign.astype(jnp.bfloat16),
        normed_ref[...],
        (((0,), (0,)), ((), ())),
        preferred_element_type=jnp.float32,
    )
    outgoing[...] = spread.astype(jnp.bfloat16).reshape(experts, capacity, width)
    rows[0, t] = outgoing[me]

    def dispatch(step):
        dst = step_partner(step, me, experts, False)
        return pltpu.make_async_remote_copy(
            src_ref=outgoing.at[dst],
            dst_ref=rows.at[step, t],
            send_sem=disp_send.at[step],
            recv_sem=disp_recv.at[step],
            device_id={"sp": dst},
            device_id_type=MESH,
        )

    def forward(step, d):
        dst = (t + d) % tps
        return pltpu.make_async_remote_copy(
            src_ref=rows.at[step, t],
            dst_ref=rows.at[step, t],
            send_sem=fwd_send.at[step, d],
            recv_sem=fwd_recv.at[step, d],
            device_id={"tp": dst},
            device_id_type=MESH,
        )

    def share(step, d):
        dst = (t + d) % tps
        return pltpu.make_async_remote_copy(
            src_ref=part.at[step, dst],
            dst_ref=peer.at[step, d],
            send_sem=part_send.at[step, d],
            recv_sem=part_recv.at[step, d],
            device_id={"tp": dst},
            device_id_type=MESH,
        )

    def give_back(step):
        dst = step_partner(step, me, experts, True)
        return pltpu.make_async_remote_copy(
            src_ref=summed.at[step],
            dst_ref=returned.at[me],
            send_sem=ret_send.at[step],
            recv_sem=ret_recv.at[step],
            device_id={"sp": dst},
            device_id_type=MESH,
        )

    for step in range(1, experts):
        dispatch(step).start()

    def send_on(step):
        if step > 0:
            dispatch(step).wait_recv()
        for d in range(1, tps):
            forward(step, d).start()

    def finish(step):
        total = part[step, t].astype(jnp.float32)
        for d in range(1, tps):
            share(step, d).wait_recv()
            total = total + peer[step, d].astype(jnp.float32)
        if step == 0:
            returned[me] = total.astype(jnp.bfloat16)
        else:
            summed[step] = total.astype(jnp.bfloat16)
            give_back(step).start()

    tile = 256
    hidden_width = gate_w.shape[1]
    m = chunk * tps * capacity
    chunks = experts // chunk

    for c in range(chunks):
        k0, k1 = c * chunk, (c + 1) * chunk
        for step in range(k0, k1):
            send_on(step)
        for step in range(k0, k1):
            for d in range(1, tps):
                forward(step, d).wait_recv()
        if c == 0:
            weight_copies[0].wait()
            weight_copies[1].wait()

        def up_tile(i, carry):
            cols = pl.ds(pl.multiple_of(i * tile, tile), tile)
            block = rows[k0:k1].reshape(m, width)
            gate = jnp.dot(block, gate_w[:, cols], preferred_element_type=jnp.float32)
            up = jnp.dot(block, up_w[:, cols], preferred_element_type=jnp.float32)
            hidden[:, cols] = (gate / (1.0 + jnp.exp(-gate)) * up).astype(jnp.bfloat16)
            return carry

        lax.fori_loop(0, hidden_width // tile, up_tile, 0)
        if c == 0:
            weight_copies[2].wait()

        def down_tile(i, carry):
            cols = pl.ds(pl.multiple_of(i * tile, tile), tile)
            result = jnp.dot(hidden[...], down_w[:, cols], preferred_element_type=jnp.float32)
            part[k0:k1, :, :, cols] = result.astype(jnp.bfloat16).reshape(
                chunk, tps, capacity, tile
            )
            return carry

        lax.fori_loop(0, width // tile, down_tile, 0)
        for step in range(k0, k1):
            for d in range(1, tps):
                share(step, d).start()
        if c > 0:
            for step in range(k0 - chunk, k0):
                finish(step)
    for step in range(experts - chunk, experts):
        finish(step)
    for step in range(1, experts):
        src = step_partner(step, me, experts, False)
        pltpu.make_async_remote_copy(
            src_ref=summed.at[step],
            dst_ref=returned.at[src],
            send_sem=ret_send.at[step],
            recv_sem=ret_recv.at[step],
            device_id={"sp": src},
            device_id_type=MESH,
        ).wait_recv()

    back = returned[...].reshape(lanes, width)
    high = combine.astype(jnp.bfloat16)
    low = (combine - high.astype(jnp.float32)).astype(jnp.bfloat16)
    moe_sum = jnp.dot(high, back, preferred_element_type=jnp.float32)
    moe_sum = moe_sum + jnp.dot(low, back, preferred_element_type=jnp.float32)
    pre_final = residual_scale * normed_ref[...].astype(jnp.float32) + moe_sum
    out_ref[...] = layer_norm(pre_final, gain_ref[...], bias_ref[...]).astype(jnp.bfloat16)

    for d in range(1, tps):
        head_copy(d, t, tps, head_part, head_peer, head_send, head_recv).wait_send()
    for step in range(experts):
        if step > 0:
            dispatch(step).wait_send()
            give_back(step).wait_send()
        for d in range(1, tps):
            forward(step, d).wait_send()
            share(step, d).wait_send()


def per_device(
    resid,
    queries,
    keys,
    values,
    doc_ids,
    sink_logits,
    out_proj,
    norm1_gain,
    norm1_bias,
    route_ids,
    route_weights,
    expert_gate,
    expert_up,
    expert_down,
    norm2_gain,
    norm2_bias,
):
    experts, tps = lax.axis_size("sp"), lax.axis_size("tp")
    toks, width = resid.shape
    tok_dev, kv_width = keys.shape
    need = 5 * toks // (2 * experts)
    capacity = -(-need // 16) * 16
    chunk = experts // CHUNKS
    hidden_width = expert_gate.shape[2]
    reach = -(-(toks + 2 * WINDOW) // 128) * 128
    padded = (tps - 1) * toks + reach
    docs = jnp.broadcast_to(doc_ids[:, None], (tok_dev, 128))
    vmem = pl.BlockSpec(memory_space=pltpu.VMEM)
    hbm = pl.BlockSpec(memory_space=pl.ANY)
    bf16 = jnp.bfloat16
    dma = pltpu.SemaphoreType.DMA
    return pl.pallas_call(
        functools.partial(layer_kernel, experts, tps, chunk),
        out_shape=jax.ShapeDtypeStruct((toks, width), bf16),
        in_specs=[vmem] * 11 + [hbm] * 5,
        out_specs=vmem,
        scratch_shapes=[
            pltpu.VMEM((toks, width), bf16),
            pltpu.VMEM(out_proj.shape, bf16),
            pltpu.VMEM((padded, kv_width), bf16),
            pltpu.VMEM((padded, kv_width), bf16),
            pltpu.VMEM((padded, 128), jnp.int32),
            pltpu.VMEM((toks, queries.shape[1]), bf16),
            pltpu.VMEM((tps, toks, width), bf16),
            pltpu.VMEM((tps, toks, width), bf16),
            pltpu.VMEM((toks, width), bf16),
            pltpu.VMEM((experts, capacity, width), bf16),
            pltpu.VMEM((experts, tps, capacity, width), bf16),
            pltpu.VMEM((width, hidden_width), bf16),
            pltpu.VMEM((width, hidden_width), bf16),
            pltpu.VMEM((hidden_width, width), bf16),
            pltpu.VMEM((chunk * tps * capacity, hidden_width), bf16),
            pltpu.VMEM((experts, tps, capacity, width), bf16),
            pltpu.VMEM((experts, tps, capacity, width), bf16),
            pltpu.VMEM((experts, capacity, width), bf16),
            pltpu.VMEM((experts, capacity, width), bf16),
            dma((5,)),
            dma((experts,)),
            dma((experts,)),
            dma((experts, tps)),
            dma((experts, tps)),
            dma((experts, tps)),
            dma((experts, tps)),
            dma((experts,)),
            dma((experts,)),
            dma((6,)),
            dma((6,)),
            dma((tps,)),
            dma((tps,)),
        ],
        compiler_params=pltpu.CompilerParams(
            collective_id=0, has_side_effects=True, vmem_limit_bytes=60 * 1024 * 1024
        ),
    )(
        queries,
        keys,
        values,
        docs,
        sink_logits[None, :],
        norm1_gain[None, :],
        norm1_bias[None, :],
        route_ids,
        route_weights,
        norm2_gain[None, :],
        norm2_bias[None, :],
        resid,
        out_proj,
        expert_gate,
        expert_up,
        expert_down,
    )


def solution(mesh):
    return jax.shard_map(
        per_device,
        mesh=mesh,
        in_specs=(
            P(("grp", "sp", "tp"), None),
            P(("grp", "sp"), "tp"),
            P(("grp", "sp"), "tp"),
            P(("grp", "sp"), "tp"),
            P(("grp", "sp")),
            P("tp"),
            P("tp", None),
            P(),
            P(),
            P(("grp", "sp", "tp"), None),
            P(("grp", "sp", "tp"), None),
            P("sp", None, "tp"),
            P("sp", None, "tp"),
            P("sp", "tp", None),
            P(),
            P(),
        ),
        out_specs=P(("grp", "sp", "tp"), None),
        check_vma=False,
    )
```

```python
import functools

import jax
import jax.numpy as jnp
from jax import lax
from jax.experimental import pallas as pl
from jax.experimental.pallas import tpu as pltpu
from jax.sharding import PartitionSpec as P

HEAD_DIM = 64
WINDOW = 128
MESH = pl.DeviceIdType.MESH
CHUNKS = 4


norm_epsilon = 1e-05
residual_scale = 1.4142135623730951
masked_score = -1e30


def layer_norm(values, gain_vec, bias_vec):
    mean_val = jnp.mean(values, -1, keepdims=True)
    centred = values - mean_val
    variance = jnp.mean(centred * centred, -1, keepdims=True)
    return centred * lax.rsqrt(variance + norm_epsilon) * gain_vec + bias_vec


def step_partner(step, sp_pos, count, back):
    chip, core = sp_pos // 2, sp_pos % 2
    half = count // 4
    side, place = chip // half, chip % half
    pair, flip = step // 2, step % 2
    if pair == 0:
        turn, cross = 0, False
    elif pair <= half:
        turn, cross = pair - 1, True
    else:
        turn, cross = pair - half, False
    target_side = 1 - side if cross else side
    move = half - turn if back else turn
    target = target_side * half + (place + move) % half
    return target * 2 + (core + flip) % 2


def head_copy(d, t, tps, head_part, head_peer, head_send, head_recv):
    return pltpu.make_async_remote_copy(
        src_ref=head_part.at[d],
        dst_ref=head_peer.at[d],
        send_sem=head_send.at[d],
        recv_sem=head_recv.at[d],
        device_id={"tp": (t + d) % tps},
        device_id_type=MESH,
    )


def attend(
    count,
    tps,
    queries_ref,
    keys_ref,
    values_ref,
    docs_ref,
    sink_ref,
    proj_w,
    key_pad,
    value_pad,
    doc_pad,
    attended,
    head_part,
    head_peer,
    halo_send,
    halo_recv,
    head_send,
    head_recv,
    barrier,
    first_copies,
):
    me, t = lax.axis_index("sp"), lax.axis_index("tp")
    tok_dev, tok_sub = queries_ref.shape[0], attended.shape[0]
    local_kv = keys_ref.shape[1] // HEAD_DIM
    heads = queries_ref.shape[1] // HEAD_DIM
    groups = heads // local_kv
    reach = -(-(tok_sub + 2 * WINDOW) // 128) * 128
    end = WINDOW + tok_dev
    rest = key_pad.shape[0] - end - WINDOW
    for pad, own in ((key_pad, keys_ref), (value_pad, values_ref), (doc_pad, docs_ref)):
        pad[WINDOW:end] = own[...]
        if rest:
            pad[end + WINDOW :] = jnp.zeros((rest, pad.shape[1]), pad.dtype)
    pl.semaphore_wait(barrier, count - 1 + tps - 1)
    copies = []
    for i, (pad, own) in enumerate(
        ((key_pad, keys_ref), (value_pad, values_ref), (doc_pad, docs_ref))
    ):
        for side in range(2):
            start, place = (tok_dev - WINDOW, 0) if side == 0 else (0, end)
            copies.append(
                pltpu.make_async_remote_copy(
                    src_ref=own.at[pl.ds(start, WINDOW)],
                    dst_ref=pad.at[pl.ds(place, WINDOW)],
                    send_sem=halo_send.at[2 * i + side],
                    recv_sem=halo_recv.at[2 * i + side],
                    device_id={"sp": (me + 1) % count if side == 0 else (me + count - 1) % count},
                    device_id_type=MESH,
                )
            )
    for copy in copies:
        copy.start()
    for copy in copies:
        copy.wait_recv()

    for d in list(range(1, tps)) + [0]:
        base = pl.multiple_of((t + d) % tps * tok_sub, 16)
        key_block = key_pad[pl.ds(base, reach), :].astype(jnp.float32)
        value_block = value_pad[pl.ds(base, reach), :].astype(jnp.float32)
        key_docs = jnp.transpose(doc_pad[pl.ds(base, reach), :])[0:1, :]
        query_docs = docs_ref[pl.ds(base, tok_sub), 0:1]
        row = lax.broadcasted_iota(jnp.int32, (tok_sub, reach), 0)
        col = lax.broadcasted_iota(jnp.int32, (tok_sub, reach), 1)
        position = me * tok_dev + base - WINDOW + col
        allowed = (position >= 0) & (position < count * tok_dev)
        allowed = allowed & (col >= row) & (col <= row + 2 * WINDOW)
        allowed = allowed & (query_docs == key_docs)
        blank = jnp.zeros((reach, HEAD_DIM), jnp.float32)
        for g in range(local_kv):
            span = slice(g * HEAD_DIM, (g + 1) * HEAD_DIM)
            sides = []
            for block in (key_block, value_block):
                piece = block[:, span]
                sides.append(
                    [
                        jnp.concatenate([piece, blank], 1).astype(jnp.bfloat16),
                        jnp.concatenate([blank, piece], 1).astype(jnp.bfloat16),
                    ]
                )
            for pair in range(groups // 2):
                lane = (g * groups + 2 * pair) * HEAD_DIM
                query = queries_ref[pl.ds(base, tok_sub), lane : lane + 2 * HEAD_DIM]
                result = jnp.zeros((tok_sub, 2 * HEAD_DIM), jnp.float32)
                for parity in range(2):
                    head = g * groups + 2 * pair + parity
                    sink = sink_ref[:, head : head + 1]
                    scores = lax.dot_general(
                        query,
                        sides[0][parity],
                        (((1,), (1,)), ((), ())),
                        preferred_element_type=jnp.float32,
                    )
                    scores = jnp.where(allowed, scores * HEAD_DIM ** (-0.5), masked_score)
                    top = jnp.maximum(jnp.max(scores, -1, keepdims=True), sink)
                    raised = jnp.where(allowed, jnp.exp(scores - top), 0.0)
                    total = jnp.exp(sink - top) + jnp.sum(raised, -1, keepdims=True)
                    weights = (raised / total).astype(jnp.bfloat16)
                    result = result + jnp.dot(
                        weights, sides[1][parity], preferred_element_type=jnp.float32
                    )
                attended[:, lane : lane + 2 * HEAD_DIM] = result.astype(jnp.bfloat16)
        if d == 1 or tps == 1:
            for copy in first_copies:
                copy.wait()
        tile = 512
        width = proj_w.shape[1]

        def project(i, carry):
            cols = pl.ds(pl.multiple_of(i * tile, tile), tile)
            head_part[d, :, cols] = jnp.dot(
                attended[...], proj_w[:, cols], preferred_element_type=jnp.float32
            ).astype(jnp.bfloat16)
            return carry

        lax.fori_loop(0, width // tile, project, 0)
        if d:
            head_copy(d, t, tps, head_part, head_peer, head_send, head_recv).start()
    for copy in copies:
        copy.wait_send()


def layer_kernel(
    experts,
    tps,
    chunk,
    queries_ref,
    keys_ref,
    values_ref,
    docs_ref,
    sink_ref,
    gain1_ref,
    bias1_ref,
    route_ref,
    gain_ref,
    bias_ref,
    resid_hbm,
    proj_hbm,
    gate_hbm,
    up_hbm,
    down_hbm,
    out_ref,
    resid_ref,
    proj_w,
    key_pad,
    value_pad,
    doc_pad,
    attended,
    head_part,
    head_peer,
    normed_ref,
    outgoing,
    rows,
    gate_w,
    up_w,
    down_w,
    hidden,
    part,
    peer,
    summed,
    returned,
    w_sem,
    disp_send,
    disp_recv,
    fwd_send,
    fwd_recv,
    part_send,
    part_recv,
    ret_send,
    ret_recv,
    halo_send,
    halo_recv,
    head_send,
    head_recv,
):
    me, t = lax.axis_index("sp"), lax.axis_index("tp")
    _, capacity, width = outgoing.shape
    toks = normed_ref.shape[0]
    first_copies = [
        pltpu.make_async_copy(resid_hbm, resid_ref, w_sem.at[3]),
        pltpu.make_async_copy(proj_hbm, proj_w, w_sem.at[4]),
    ]
    for copy in first_copies:
        copy.start()
    weight_copies = [
        pltpu.make_async_copy(gate_hbm.at[0], gate_w, w_sem.at[0]),
        pltpu.make_async_copy(up_hbm.at[0], up_w, w_sem.at[1]),
        pltpu.make_async_copy(down_hbm.at[0], down_w, w_sem.at[2]),
    ]
    for copy in weight_copies:
        copy.start()

    barrier = pltpu.get_barrier_semaphore()
    for d in range(1, experts):
        pl.semaphore_signal(
            barrier, inc=1, device_id={"sp": (me + d) % experts}, device_id_type=MESH
        )
    for d in range(1, tps):
        pl.semaphore_signal(barrier, inc=1, device_id={"tp": (t + d) % tps}, device_id_type=MESH)

    attend(
        experts,
        tps,
        queries_ref,
        keys_ref,
        values_ref,
        docs_ref,
        sink_ref,
        proj_w,
        key_pad,
        value_pad,
        doc_pad,
        attended,
        head_part,
        head_peer,
        halo_send,
        halo_recv,
        head_send,
        head_recv,
        barrier,
        first_copies,
    )
    lanes = experts * capacity
    top = route_ref.shape[1] // 2
    ids = route_ref[:, :top].astype(jnp.int32)
    wide = max(experts, 128)
    expert_iota = lax.broadcasted_iota(jnp.int32, (toks, wide), 1)
    lower = (
        lax.broadcasted_iota(jnp.int32, (toks, toks), 0)
        > lax.broadcasted_iota(jnp.int32, (toks, toks), 1)
    ).astype(jnp.float32).astype(jnp.bfloat16)
    before = jnp.zeros((1, wide), jnp.float32)
    slot_iota = lax.broadcasted_iota(jnp.int32, (toks, lanes), 1)
    assign = jnp.zeros((toks, lanes), jnp.float32)
    combine = jnp.zeros((toks, lanes), jnp.float32)
    for k in range(ids.shape[1]):
        own = ids[:, k : k + 1]
        hot = (own == expert_iota).astype(jnp.float32)
        rank = before + jnp.dot(lower, hot.astype(jnp.bfloat16), preferred_element_type=jnp.float32)
        rank = jnp.sum(rank * hot, axis=1, keepdims=True).astype(jnp.int32)
        before = before + jnp.sum(hot, axis=0, keepdims=True)
        match = (own * capacity + rank == slot_iota).astype(jnp.float32)
        assign = assign + match
        combine = combine + match * route_ref[:, top + k : top + k + 1]
    projected = head_part[0].astype(jnp.float32)
    for d in range(1, tps):
        head_copy(d, t, tps, head_part, head_peer, head_send, head_recv).wait_recv()
        projected = projected + head_peer[d].astype(jnp.float32)
    projected = projected.astype(jnp.bfloat16).astype(jnp.float32)
    pre_norm = residual_scale * resid_ref[...].astype(jnp.float32) + projected
    normed_ref[...] = layer_norm(pre_norm, gain1_ref[...], bias1_ref[...]).astype(jnp.bfloat16)
    spread = lax.dot_general(
        assign.astype(jnp.bfloat16),
        normed_ref[...],
        (((0,), (0,)), ((), ())),
        preferred_element_type=jnp.float32,
    )
    outgoing[...] = spread.astype(jnp.bfloat16).reshape(experts, capacity, width)
    rows[0, t] = outgoing[me]

    def dispatch(step):
        dst = step_partner(step, me, experts, False)
        return pltpu.make_async_remote_copy(
            src_ref=outgoing.at[dst],
            dst_ref=rows.at[step, t],
            send_sem=disp_send.at[step],
            recv_sem=disp_recv.at[step],
            device_id={"sp": dst},
            device_id_type=MESH,
        )

    def forward(step, d):
        dst = (t + d) % tps
        return pltpu.make_async_remote_copy(
            src_ref=rows.at[step, t],
            dst_ref=rows.at[step, t],
            send_sem=fwd_send.at[step, d],
            recv_sem=fwd_recv.at[step, d],
            device_id={"tp": dst},
            device_id_type=MESH,
        )

    def share(step, d):
        dst = (t + d) % tps
        return pltpu.make_async_remote_copy(
            src_ref=part.at[step, dst],
            dst_ref=peer.at[step, d],
            send_sem=part_send.at[step, d],
            recv_sem=part_recv.at[step, d],
            device_id={"tp": dst},
            device_id_type=MESH,
        )

    def give_back(step):
        dst = step_partner(step, me, experts, True)
        return pltpu.make_async_remote_copy(
            src_ref=summed.at[step],
            dst_ref=returned.at[me],
            send_sem=ret_send.at[step],
            recv_sem=ret_recv.at[step],
            device_id={"sp": dst},
            device_id_type=MESH,
        )

    for step in range(1, experts):
        dispatch(step).start()

    def send_on(step):
        if step > 0:
            dispatch(step).wait_recv()
        for d in range(1, tps):
            forward(step, d).start()

    def finish(step):
        total = part[step, t].astype(jnp.float32)
        for d in range(1, tps):
            share(step, d).wait_recv()
            total = total + peer[step, d].astype(jnp.float32)
        if step == 0:
            returned[me] = total.astype(jnp.bfloat16)
        else:
            summed[step] = total.astype(jnp.bfloat16)
            give_back(step).start()

    tile = 512 if gate_w.shape[1] % 512 == 0 else 256
    hidden_width = gate_w.shape[1]
    m = chunk * tps * capacity
    chunks = experts // chunk

    for c in range(chunks):
        k0, k1 = c * chunk, (c + 1) * chunk
        if c == 0:
            for step in range(k0, k1):
                send_on(step)
        for step in range(k0, k1):
            for d in range(1, tps):
                forward(step, d).wait_recv()
        if c == 0:
            weight_copies[0].wait()
            weight_copies[1].wait()

        def up_tile(i, carry):
            cols = pl.ds(pl.multiple_of(i * tile, tile), tile)
            block = rows[k0:k1].reshape(m, width)
            gate = jnp.dot(block, gate_w[:, cols], preferred_element_type=jnp.float32)
            up = jnp.dot(block, up_w[:, cols], preferred_element_type=jnp.float32)
            hidden[:, cols] = (gate / (1.0 + jnp.exp(-gate)) * up).astype(jnp.bfloat16)
            return carry

        lax.fori_loop(0, hidden_width // tile, up_tile, 0)
        if c + 1 < chunks:
            for step in range(k1, k1 + chunk):
                send_on(step)
        if c == 0:
            weight_copies[2].wait()

        def down_tile(i, carry):
            cols = pl.ds(pl.multiple_of(i * tile, tile), tile)
            result = jnp.dot(hidden[...], down_w[:, cols], preferred_element_type=jnp.float32)
            part[k0:k1, :, :, cols] = result.astype(jnp.bfloat16).reshape(
                chunk, tps, capacity, tile
            )
            return carry

        lax.fori_loop(0, width // tile, down_tile, 0)
        for step in range(k0, k1):
            for d in range(1, tps):
                share(step, d).start()
        if c > 0:
            for step in range(k0 - chunk, k0):
                finish(step)
    for step in range(experts - chunk, experts):
        finish(step)
    for step in range(1, experts):
        src = step_partner(step, me, experts, False)
        pltpu.make_async_remote_copy(
            src_ref=summed.at[step],
            dst_ref=returned.at[src],
            send_sem=ret_send.at[step],
            recv_sem=ret_recv.at[step],
            device_id={"sp": src},
            device_id_type=MESH,
        ).wait_recv()

    back = returned[...].reshape(lanes, width)
    high = combine.astype(jnp.bfloat16)
    low = (combine - high.astype(jnp.float32)).astype(jnp.bfloat16)
    moe_sum = jnp.dot(high, back, preferred_element_type=jnp.float32)
    moe_sum = moe_sum + jnp.dot(low, back, preferred_element_type=jnp.float32)
    pre_final = residual_scale * normed_ref[...].astype(jnp.float32) + moe_sum
    out_ref[...] = layer_norm(pre_final, gain_ref[...], bias_ref[...]).astype(jnp.bfloat16)

    for d in range(1, tps):
        head_copy(d, t, tps, head_part, head_peer, head_send, head_recv).wait_send()
    for step in range(experts):
        if step > 0:
            dispatch(step).wait_send()
            give_back(step).wait_send()
        for d in range(1, tps):
            forward(step, d).wait_send()
            share(step, d).wait_send()


def per_device(
    resid,
    queries,
    keys,
    values,
    doc_ids,
    sink_logits,
    out_proj,
    norm1_gain,
    norm1_bias,
    route_ids,
    route_weights,
    expert_gate,
    expert_up,
    expert_down,
    norm2_gain,
    norm2_bias,
):
    experts, tps = lax.axis_size("sp"), lax.axis_size("tp")
    toks, width = resid.shape
    tok_dev, kv_width = keys.shape
    need = 5 * toks // (2 * experts)
    capacity = -(-need // 16) * 16
    chunk = experts // CHUNKS
    hidden_width = expert_gate.shape[2]
    reach = -(-(toks + 2 * WINDOW) // 128) * 128
    padded = (tps - 1) * toks + reach
    docs = jnp.broadcast_to(doc_ids[:, None], (tok_dev, 128))
    routes = jnp.concatenate([route_ids.astype(jnp.float32), route_weights], 1)
    vmem = pl.BlockSpec(memory_space=pltpu.VMEM)
    hbm = pl.BlockSpec(memory_space=pl.ANY)
    bf16 = jnp.bfloat16
    dma = pltpu.SemaphoreType.DMA
    return pl.pallas_call(
        functools.partial(layer_kernel, experts, tps, chunk),
        out_shape=jax.ShapeDtypeStruct((toks, width), bf16),
        in_specs=[vmem] * 10 + [hbm] * 5,
        out_specs=vmem,
        scratch_shapes=[
            pltpu.VMEM((toks, width), bf16),
            pltpu.VMEM(out_proj.shape, bf16),
            pltpu.VMEM((padded, kv_width), bf16),
            pltpu.VMEM((padded, kv_width), bf16),
            pltpu.VMEM((padded, 128), jnp.int32),
            pltpu.VMEM((toks, queries.shape[1]), bf16),
            pltpu.VMEM((tps, toks, width), bf16),
            pltpu.VMEM((tps, toks, width), bf16),
            pltpu.VMEM((toks, width), bf16),
            pltpu.VMEM((experts, capacity, width), bf16),
            pltpu.VMEM((experts, tps, capacity, width), bf16),
            pltpu.VMEM((width, hidden_width), bf16),
            pltpu.VMEM((width, hidden_width), bf16),
            pltpu.VMEM((hidden_width, width), bf16),
            pltpu.VMEM((chunk * tps * capacity, hidden_width), bf16),
            pltpu.VMEM((experts, tps, capacity, width), bf16),
            pltpu.VMEM((experts, tps, capacity, width), bf16),
            pltpu.VMEM((experts, capacity, width), bf16),
            pltpu.VMEM((experts, capacity, width), bf16),
            dma((5,)),
            dma((experts,)),
            dma((experts,)),
            dma((experts, tps)),
            dma((experts, tps)),
            dma((experts, tps)),
            dma((experts, tps)),
            dma((experts,)),
            dma((experts,)),
            dma((6,)),
            dma((6,)),
            dma((tps,)),
            dma((tps,)),
        ],
        compiler_params=pltpu.CompilerParams(
            collective_id=0, has_side_effects=True, vmem_limit_bytes=60 * 1024 * 1024
        ),
    )(
        queries,
        keys,
        values,
        docs,
        sink_logits[None, :],
        norm1_gain[None, :],
        norm1_bias[None, :],
        routes,
        norm2_gain[None, :],
        norm2_bias[None, :],
        resid,
        out_proj,
        expert_gate,
        expert_up,
        expert_down,
    )


def solution(mesh):
    return jax.shard_map(
        per_device,
        mesh=mesh,
        in_specs=(
            P(("grp", "sp", "tp"), None),
            P(("grp", "sp"), "tp"),
            P(("grp", "sp"), "tp"),
            P(("grp", "sp"), "tp"),
            P(("grp", "sp")),
            P("tp"),
            P("tp", None),
            P(),
            P(),
            P(("grp", "sp", "tp"), None),
            P(("grp", "sp", "tp"), None),
            P("sp", None, "tp"),
            P("sp", None, "tp"),
            P("sp", "tp", None),
            P(),
            P(),
        ),
        out_specs=P(("grp", "sp", "tp"), None),
        check_vma=False,
    )
```
